128 devices in a mesh: sp: 16 (over z, y), dp: 8 (over x, core).
Axes of the slice: x: 4, y: 4, z: 4, core: 2. Of those that a mesh axis runs over, the one named last changes fastest.
Arguments:
- queries: bfloat16 [8, 2048, 2048], P('dp', 'sp'), may hold values from -40 to 40
- keys: bfloat16 [8, 2048, 512], P('dp', 'sp'), may hold values from -8 to 8
- values: bfloat16 [8, 2048, 512], P('dp', 'sp'), may hold values from -6 to 6
- lambdas: float32 [16], replicated, may hold values from 0.3 to 0.8
- value_gain: float32 [128], replicated, may hold values from 0.1 to 1.9
- out_weight: bfloat16 [2048, 4096], P(None, ('sp', 'dp')), may hold values from -0.125 to 0.125
Outputs:
- mixed: bfloat16 [8, 2048, 4096], P('dp', 'sp')
The draws below stay inside these ranges and needn't reach their ends.
All inputs are finite; a program needn't handle non-finite values.
Results may differ from the reference program's by a relative error of at most 0.0087.
Values may be sent and summed in bfloat16 or wider, within the bound.
No kernel may reach another device: no remote copies, remote signals or barrier semaphores. Data moves between devices by JAX's collectives and lax.ppermute only.
A program may use at most 128 MiB of HBM per device.

```python
import jax
import jax.numpy as jnp
from jax import lax

D = 4096
HEADS = 16
KV_HEADS = 4
HEAD_DIM = 64
VALUE_DIM = 128
SEQLEN = 2048
SEQS = 8


def base_keys(key):
    draw_key = jax.random.fold_in(key, 3)
    shape = (SEQS, SEQLEN, KV_HEADS, 2, HEAD_DIM)
    keys_float = jnp.clip(1.3 * jax.random.normal(draw_key, shape, jnp.float32), -8.0, 8.0)
    return keys_float


def draw_keys(key, part):
    return base_keys(key).reshape(SEQS, SEQLEN, KV_HEADS * 2 * HEAD_DIM).astype(jnp.bfloat16)


def draw_queries(key, part):
    draw_key = jax.random.fold_in(key, 4)
    shape = (SEQS, SEQLEN, HEADS, 2, HEAD_DIM)
    queries_float = jnp.clip(1.3 * jax.random.normal(draw_key, shape, jnp.float32), -8.0, 8.0)
    return queries_float.reshape(SEQS, SEQLEN, HEADS * 2 * HEAD_DIM).astype(jnp.bfloat16)


def block_levels(own_key, shape, pieces, low, high):
    loudness = 1.0
    for position, blocks in pieces:
        steps = jax.random.uniform(jax.random.fold_in(jax.random.fold_in(own_key, 6), position), (blocks,), jnp.float32, low / len(pieces), high / len(pieces))
        loudness = loudness * jnp.repeat(jnp.exp(steps), shape[position] // blocks).reshape((-1,) + (1,) * (len(shape) - 1 - position))
    return loudness


def scatter_about(own_key, extent, deviation, most, split=(), kind=jnp.bfloat16):
    result = deviation * jax.random.normal(own_key, extent, jnp.float32)
    if split:
        result = result * block_levels(own_key, extent, split, -0.22, 0.18)
    return jnp.clip(result, -most, most).astype(kind)


def setup_inputs(seed: int = 0) -> dict:
    key_of = jax.random.split(jax.random.key(seed), 7)
    queries = draw_queries(jax.random.fold_in(key_of[6], 71), 0)
    keys = draw_keys(jax.random.fold_in(key_of[6], 71), 0)
    values = scatter_about(key_of[2], (SEQS, SEQLEN, KV_HEADS * VALUE_DIM), 1.0, 6.0, ((0, 8), (1, 16)))
    lambdas = jnp.clip(jax.random.uniform(key_of[3], (HEADS,), jnp.float32, 0.3, 0.8), 0.3, 0.8)
    value_gain = jnp.clip(1.0 + 0.18 * jax.random.normal(key_of[4], (VALUE_DIM,), jnp.float32), 0.1, 1.9)
    out_weight = scatter_about(key_of[5], (HEADS * VALUE_DIM, D), (HEADS * VALUE_DIM) ** -0.5, 0.125, ((1, 128),))
    return {"queries": queries, "keys": keys, "values": values, "lambdas": lambdas, "value_gain": value_gain, "out_weight": out_weight}


rope_base = 500000.0
output_scale = 0.8
norm_eps = 1e-05

def rotate_all(parts, positions):
    width = parts.shape[-1]
    half = width // 2
    freqs = rope_base ** (-jnp.arange(0, width, 2, dtype=jnp.float32) / width)
    angles = positions[:, None] * freqs[None, :]
    shape = (1, angles.shape[0], 1, 1, half)
    cosine = jnp.cos(angles).reshape(shape)
    sine = jnp.sin(angles).reshape(shape)
    first = parts[..., :half]
    second = parts[..., half:]
    return jnp.concatenate([first * cosine - second * sine, second * cosine + first * sine], -1)

def reference(queries, keys, values, lambdas, value_gain, out_weight):
    positions = jnp.arange(SEQLEN, dtype=jnp.float32)
    query_rot = rotate_all(queries.astype(jnp.float32).reshape(SEQS, SEQLEN, HEADS, 2, HEAD_DIM), positions).astype(jnp.bfloat16)
    key_rot = rotate_all(keys.astype(jnp.float32).reshape(SEQS, SEQLEN, KV_HEADS, 2, HEAD_DIM), positions).astype(jnp.bfloat16)
    value_parts = values.reshape(SEQS, SEQLEN, KV_HEADS, VALUE_DIM)
    group_size = HEADS // KV_HEADS
    key_heads = jnp.repeat(key_rot, group_size, axis=2)
    value_heads = jnp.repeat(value_parts, group_size, axis=2)
    query_flat = jnp.transpose(query_rot, (0, 2, 1, 3, 4)).reshape(SEQS * HEADS, SEQLEN, 2, HEAD_DIM)
    key_flat = jnp.transpose(key_heads, (0, 2, 1, 3, 4)).reshape(SEQS * HEADS, SEQLEN, 2, HEAD_DIM)
    value_flat = jnp.transpose(value_heads, (0, 2, 1, 3)).reshape(SEQS * HEADS, SEQLEN, VALUE_DIM)
    lambda_flat = jnp.tile(lambdas, SEQS)
    block_rows = min(512, SEQLEN)
    count = SEQLEN // block_rows
    score_scale = HEAD_DIM ** (-0.5)
    key_places = jnp.arange(SEQLEN)

    def one_head(inputs):
        query_one, key_one, value_one, lambda_one = inputs

        def one_block(block_index):
            start = block_index * block_rows
            query_block = lax.dynamic_slice_in_dim(query_one, start, block_rows, 0)
            scores = jnp.einsum('qmd,kmd->mqk', query_block.astype(jnp.float32), key_one.astype(jnp.float32)) * score_scale
            allowed = key_places[None, :] <= (start + jnp.arange(block_rows))[:, None]
            scores = jnp.where(allowed[None], scores, -jnp.inf)
            row_top = lax.optimization_barrier(jnp.max(scores, -1, keepdims=True))
            raised = jnp.exp(scores - row_top)
            maps = raised / lax.optimization_barrier(jnp.sum(raised, -1, keepdims=True))
            weights = (maps[0] - lambda_one * maps[1]).astype(jnp.bfloat16)
            return jnp.dot(weights, value_one, preferred_element_type=jnp.float32)
        blocks = lax.map(one_block, jnp.arange(count))
        head_values = blocks.reshape(SEQLEN, VALUE_DIM)
        squares = lax.optimization_barrier(jnp.mean(head_values * head_values, -1, keepdims=True))
        return (head_values * lax.rsqrt(squares + norm_eps) * value_gain * output_scale).astype(jnp.bfloat16)
    head_out = lax.map(one_head, (query_flat, key_flat, value_flat, lambda_flat))
    heads_out = jnp.transpose(head_out.reshape(SEQS, HEADS, SEQLEN, VALUE_DIM), (0, 2, 1, 3)).reshape(SEQS * SEQLEN, HEADS * VALUE_DIM)
    mixed = jnp.dot(heads_out, out_weight, preferred_element_type=jnp.float32).astype(jnp.bfloat16)
    return mixed.reshape(SEQS, SEQLEN, D)
```

```python
import functools

import jax
import jax.numpy as jnp
from jax import lax
from jax.experimental import pallas as pl
from jax.experimental.pallas import tpu as pltpu
from jax.sharding import Mesh
from jax.sharding import PartitionSpec as P


F32 = jnp.float32
BF16 = jnp.bfloat16
HEAD_DIM = 64
ROPE_BASE = 500000.0
OUTPUT_SCALE = 0.8
NORM_EPS = 1e-05
BLOCK = 128
SEQ = 2048
PARTS = 2

VM = pl.BlockSpec(memory_space=pltpu.VMEM)
SM = pl.BlockSpec(memory_space=pltpu.SMEM)


def cost(flops, size):
    return pl.CostEstimate(flops=flops, bytes_accessed=size, transcendentals=0)


def room(mib):
    return pltpu.CompilerParams(vmem_limit_bytes=mib * 1024 * 1024)


def shape(*dims):
    return jax.ShapeDtypeStruct(dims, BF16)


def hop(axis, step, x):
    return lax.ppermute(x, axis, [(i, (i + step) % 4) for i in range(4)])


def line(axis, x):
    return x, hop(axis, 1, x), hop(axis, 3, x), hop(axis, 2, x)


ORDER = (0, 3, 1, 2)


def rotate_kernel(lambdas, gain_ref, q_ref, k_ref, v_ref, w_ref, cos_ref, sin_ref, kv_out, w_out, const_out, *q_out):
    z = lax.axis_index("z")
    const_out[:1] = gain_ref[...]
    for h in range(4):
        const_out[h + 1 : h + 2] = jnp.full((1, 128), lambdas[z * 4 + h], F32)
    const_out[5:] = jnp.zeros((3, 128), F32)
    w_out[...] = w_ref[...]
    cosine = cos_ref[...]
    sine = sin_ref[...]
    lane = lax.broadcasted_iota(jnp.int32, (BLOCK, 128), 1)
    low = (lane % HEAD_DIM) < HEAD_DIM // 2

    def turn(x):
        x = x.astype(F32)
        other = jnp.where(low, pltpu.roll(x, 96, 1), pltpu.roll(x, 32, 1))
        return (x * cosine + other * sine).astype(BF16)

    for g in range(4):
        kv_out[g, :, :128] = turn(k_ref[0, :, g * 128 : (g + 1) * 128])
        kv_out[g, :, 128:] = v_ref[0, :, g * 128 : (g + 1) * 128]
    for r in range(4):
        group = lax.rem(z + r, 4) * 512
        for h in range(4):
            at = pl.multiple_of(group + h * 128, 128)
            q_out[r][:, h * 128 : (h + 1) * 128] = turn(q_ref[0, :, pl.ds(at, 128)]) * BF16(0.125)


def rotate(lambdas, gain, q, k, v, w, cosine, sine):
    return pl.pallas_call(
        rotate_kernel,
        in_specs=[SM] + [VM] * 7,
        out_specs=[VM] * 7,
        out_shape=[shape(4, BLOCK, 256), shape(*w.shape), jax.ShapeDtypeStruct((8, 128), F32)]
        + [shape(BLOCK, 512)] * 4,
        cost_estimate=cost(2**20, 2**20),
        compiler_params=room(8),
        name="rotate",
    )(lambdas, gain, q, k, v, w, cosine, sine)


def attend_kernel(rows, const, *refs):
    z = lax.axis_index("z")
    y = lax.axis_index("y")
    gain = const[:1]
    q_refs, refs = refs[:4], refs[4:]
    if len(refs) == 8:
        kv_refs, (out_ref, kbuf, vbuf, q_ref) = refs[:4], refs[4:]
        for r, ref in enumerate(kv_refs):
            src = lax.rem(y + ORDER[r], 4)
            for j in range(4):
                at = pl.multiple_of(j * 512 + src * 128, 128)
                kbuf[:, pl.ds(at, 128)] = ref[j, :, :128].T
                vbuf[pl.ds(at, 128), :] = ref[j, :, 128:]
    else:
        kbuf, vbuf, out_ref, q_ref = refs
    for r, ref in enumerate(q_refs):
        q_ref[lax.rem(z + 4 - r, 4)] = ref[rows, :]
    count = rows.stop - rows.start
    heads = BLOCK // count
    first = lax.broadcasted_iota(jnp.int32, (count, 128), 1) < HEAD_DIM
    zero = jnp.zeros((count, 128), BF16)
    key_at = lax.broadcasted_iota(jnp.int32, (2 * BLOCK, 512), 1)
    query_at = lax.broadcasted_iota(jnp.int32, (2 * BLOCK, 512), 0) % count + rows.start
    allowed = key_at <= query_at + y * BLOCK
    row_head = lax.broadcasted_iota(jnp.int32, (BLOCK, 1), 0) // count

    for i in range(4):
        reach = (i + 1) * 512
        for g in range(4 // heads):
            qs = [q_ref[i, :, h * 128 : (h + 1) * 128] for h in range(g * heads, (g + 1) * heads)]
            q = jnp.concatenate([jnp.where(first, q, zero) for q in qs] + [jnp.where(first, zero, q) for q in qs], 0)
            last = jnp.dot(q, kbuf[:, reach - 512 : reach], preferred_element_type=F32)
            last = jnp.where(allowed, last, -jnp.inf)
            top = jnp.max(last, 1, keepdims=True)
            if i:
                rest = jnp.dot(q, kbuf[:, : reach - 512], preferred_element_type=F32)
                top = jnp.maximum(top, jnp.max(rest, 1, keepdims=True))
                rest = jnp.exp(rest - top)
            last = jnp.exp(last - top)
            total = jnp.sum(last, 1, keepdims=True)
            if i:
                total = total + jnp.sum(rest, 1, keepdims=True)
            scale = 1.0 / total
            one = scale[:BLOCK]
            factor = const[g * heads + 1 : g * heads + 2, :1]
            if heads == 2:
                factor = jnp.where(row_head == 0, factor, const[g * heads + 2 : g * heads + 3, :1])
            two = scale[BLOCK:] * factor
            w = (last[:BLOCK] * one - last[BLOCK:] * two).astype(BF16)
            acc = jnp.dot(w, vbuf[reach - 512 : reach], preferred_element_type=F32)
            if i:
                w = (rest[:BLOCK] * one - rest[BLOCK:] * two).astype(BF16)
                acc = acc + jnp.dot(w, vbuf[: reach - 512], preferred_element_type=F32)
            square = jnp.mean(acc * acc, 1, keepdims=True)
            acc = acc * (lax.rsqrt(square + NORM_EPS) * OUTPUT_SCALE) * gain
            acc = acc.astype(BF16)
            for k in range(heads):
                h = g * heads + k
                out_ref[i * count : (i + 1) * count, h * 128 : (h + 1) * 128] = acc[k * count : (k + 1) * count]


def attend(rows, const, q, keys):
    count = rows.stop - rows.start
    outs = [shape(4 * count, 512)]
    if len(keys) == 4:
        outs += [shape(128, SEQ), shape(SEQ, 128)]
    return pl.pallas_call(
        functools.partial(attend_kernel, rows),
        in_specs=[VM] * (5 + len(keys)),
        out_specs=[VM] * len(outs),
        out_shape=outs,
        scratch_shapes=[pltpu.VMEM((4, count, 512), BF16)],
        compiler_params=room(16),
        cost_estimate=cost(2**31, 2**22),
        name="attend",
    )(const, *q, *keys)


ANY = pl.BlockSpec(memory_space=pl.ANY)


def stack_kernel(_, *refs):
    out = refs[-1]
    at = 0
    for ref in refs[:-1]:
        out[at : at + ref.shape[0]] = ref[...]
        at += ref.shape[0]


def stack(after, parts):
    rows = sum(p.shape[0] for p in parts)
    return pl.pallas_call(
        stack_kernel,
        in_specs=[ANY] + [VM] * len(parts),
        out_specs=VM,
        out_shape=shape(rows, parts[0].shape[1]),
        cost_estimate=cost(2**20, 2**20),
        compiler_params=room(4),
        name="stack",
    )(after, *parts)


def columns_kernel(*refs):
    y, x, c = (lax.axis_index(a) for a in "yxc")
    wbuf = refs[-1]
    for k in range(2):
        side = c if k == 0 else 1 - c
        for a in range(4):
            ax = lax.rem(x + ORDER[a], 4)
            for b in range(4):
                by = lax.rem(y + ORDER[b], 4)
                at = pl.multiple_of(by * 256 + ax * 64 + side * 32, 32)
                wbuf[pl.ds(at, 32), :] = refs[4 * k + a][b * 32 : (b + 1) * 32, :]


def columns(parts):
    return pl.pallas_call(
        columns_kernel,
        in_specs=[VM] * 8,
        out_specs=VM,
        out_shape=shape(1024, 2048),
        compiler_params=room(12),
        cost_estimate=cost(2**29, 2**23),
        name="columns",
    )(*parts)


def project_kernel(_, x0, x1, x2, x3, wbuf, *refs):
    outs, xbuf = refs[:4], refs[4]
    z = lax.axis_index("z")
    count = x0.shape[0] // 4
    for r, ref in enumerate((x0, x1, x2, x3)):
        at = pl.multiple_of(lax.rem(z + ORDER[r], 4) * 512, 512)
        xbuf[:, pl.ds(at, 512)] = ref[...]
    for n in range(4):
        cols = slice(n * 256, (n + 1) * 256)
        part = lax.dot_general(
            xbuf[...], wbuf[cols, :], (((1,), (1,)), ((), ())), preferred_element_type=F32
        ).astype(BF16)
        for i in range(4):
            for r in range(4):

                @pl.when(lax.rem(i + 4 - z, 4) == r)
                def _():
                    outs[r][:, cols] = part[i * count : (i + 1) * count]


def project(after, xs, weights):
    rows = xs[0].shape[0]
    return pl.pallas_call(
        project_kernel,
        in_specs=[ANY] + [VM] * 5,
        out_specs=[VM] * 4,
        out_shape=[shape(rows // 4, 1024)] * 4,
        scratch_shapes=[pltpu.VMEM((rows, 2048), BF16)],
        compiler_params=room(16),
        cost_estimate=cost(2**30, 2**22),
        name="project",
    )(after, *xs, weights)


def join_kernel(*refs):
    z = lax.axis_index("z")
    for r in range(4):
        at = pl.multiple_of(lax.rem(z + 4 - r, 4) * 1024, 1024)
        refs[-1][0, :, pl.ds(at, 1024)] = refs[r][...]


def join(p, pieces, whole):
    count = pieces[0].shape[0]
    return pl.pallas_call(
        join_kernel,
        grid=(1,),
        in_specs=[pl.BlockSpec((count, 1024), lambda i: (0, 0))] * 4 + ([] if whole is None else [ANY]),
        out_specs=pl.BlockSpec((1, count, 4096), lambda i: (0, p, 0)),
        out_shape=shape(1, BLOCK, 4096),
        input_output_aliases={} if whole is None else {4: 0},
        cost_estimate=cost(2**18, 2**21),
        compiler_params=room(6),
        name="join",
    )(*pieces, *(() if whole is None else (whole,)))


def shards(queries, keys, values, lambdas, value_gain, out_weight):
    first = ((lax.axis_index("z") * 4 + lax.axis_index("y")) * BLOCK).astype(jnp.int32)
    positions = (first + jnp.arange(BLOCK)).astype(F32)
    freqs = ROPE_BASE ** (-jnp.arange(0, HEAD_DIM, 2, dtype=F32) / HEAD_DIM)
    angles = positions[:, None] * jnp.tile(freqs, 4)[None, :]
    cosine = jnp.cos(angles)
    sign = jnp.where(jnp.arange(128) % HEAD_DIM < HEAD_DIM // 2, -1.0, 1.0).astype(F32)
    sine = jnp.sin(angles) * sign[None, :]
    gain = value_gain.reshape(1, 128)
    kv_split, wt, const, *q_split = rotate(lambdas, gain, queries, keys, values, out_weight.T, cosine, sine)

    kv_line = lax.all_to_all(kv_split, "z", 0, 0)
    kv_all = line("y", kv_line)
    q = [q_split[0]] + [hop("z", r, q_split[r]) for r in (1, 2, 3)]

    wy = line("y", wt)
    wy = stack(kv_line, wy)
    wx = line("x", wy)
    wc = tuple(lax.ppermute(p, "c", [(0, 1), (1, 0)]) for p in wx)
    weights = columns(wx + wc)

    count = BLOCK // PARTS
    keys_all = kv_all
    heads = []
    for p in range(PARTS):
        got, *whole = attend(slice(p * count, (p + 1) * count), const, q, keys_all)
        keys_all = whole or keys_all
        heads.append(got)
    out = None
    for p in range(PARTS):
        got = line("z", heads[p])
        sent = project(heads[-1], got, weights)
        got = [sent[0]] + [hop("z", r, sent[r]) for r in (1, 2, 3)]
        out = join(p, got, out)
    return out


def solution(mesh):
    fine = Mesh(mesh.devices.reshape(4, 4, 4, 2), ("z", "y", "x", "c"))
    tokens = P(("x", "c"), ("z", "y"), None)
    return jax.shard_map(
        shards,
        mesh=fine,
        in_specs=(tokens, tokens, tokens, P(), P(), P(None, ("z", "y", "x", "c"))),
        out_specs=tokens,
        check_vma=False,
    )
```

```python
import functools

import jax
import jax.numpy as jnp
from jax import lax
from jax.experimental import pallas as pl
from jax.experimental.pallas import tpu as pltpu
from jax.sharding import Mesh
from jax.sharding import PartitionSpec as P


F32 = jnp.float32
BF16 = jnp.bfloat16
HEAD_DIM = 64
ROPE_BASE = 500000.0
OUTPUT_SCALE = 0.8
NORM_EPS = 1e-05
BLOCK = 128
SEQ = 2048
TILE = 256
PARTS = 2

VM = pl.BlockSpec(memory_space=pltpu.VMEM)
SM = pl.BlockSpec(memory_space=pltpu.SMEM)


def cost(flops, size):
    return pl.CostEstimate(flops=flops, bytes_accessed=size, transcendentals=0)


def room(mib):
    return pltpu.CompilerParams(vmem_limit_bytes=mib * 1024 * 1024)


def shape(*dims):
    return jax.ShapeDtypeStruct(dims, BF16)


def hop(axis, step, x):
    return lax.ppermute(x, axis, [(i, (i + step) % 4) for i in range(4)])


def line(axis, x):
    return x, hop(axis, 1, x), hop(axis, 3, x), hop(axis, 2, x)


ORDER = (0, 3, 1, 2)


HBM = pl.BlockSpec(memory_space=pltpu.HBM)


def rotate_kernel(small_ref, q_hbm, k_hbm, v_hbm, cos_ref, sin_ref, kv_out, const_out, q0, q1, q2, q3, q_ref, k_ref, sems):
    z = lax.axis_index("z")
    copies = [pltpu.make_async_copy(k_hbm.at[0], k_ref, sems.at[0])]
    for g in range(4):
        copies.append(
            pltpu.make_async_copy(v_hbm.at[0, :, pl.ds(g * 128, 128)], kv_out.at[g, :, pl.ds(128, 128)], sems.at[1 + g])
        )
    copies.append(pltpu.make_async_copy(q_hbm.at[0], q_ref, sems.at[5]))
    for copy in copies:
        copy.start()
    cosine = cos_ref[...]
    sine = sin_ref[...]
    lane = lax.broadcasted_iota(jnp.int32, (BLOCK, 128), 1)
    low = (lane % HEAD_DIM) < HEAD_DIM // 2

    def turn(x):
        x = x.astype(F32)
        other = jnp.where(low, pltpu.roll(x, 96, 1), pltpu.roll(x, 32, 1))
        return (x * cosine + other * sine).astype(BF16)

    at = lax.broadcasted_iota(jnp.int32, (8, 128), 1) - lax.broadcasted_iota(jnp.int32, (8, 128), 0)
    own = jnp.where(at == z * 4, jnp.broadcast_to(small_ref[:1], (8, 128)), 0.0)
    const_out[:8] = jnp.broadcast_to(jnp.sum(own, 1, keepdims=True), (8, 128))
    const_out[8:] = jnp.broadcast_to(small_ref[1:], (8, 128))
    copies[0].wait()
    for g in range(4):
        kv_out[g, :, :128] = turn(k_ref[:, g * 128 : (g + 1) * 128])
    copies[5].wait()
    for r, q_out in enumerate((q0, q1, q2, q3)):
        group = lax.rem(z + r, 4) * 512
        for h in range(4):
            at = pl.multiple_of(group + h * 128, 128)
            q_out[:, h * 128 : (h + 1) * 128] = turn(q_ref[:, pl.ds(at, 128)]) * BF16(0.125)
    for copy in copies[1:5]:
        copy.wait()


def rotate(small, q, k, v, cosine, sine):
    return pl.pallas_call(
        rotate_kernel,
        in_specs=[VM] + [HBM] * 3 + [VM] * 2,
        out_specs=[VM] * 6,
        out_shape=[shape(4, BLOCK, 256), jax.ShapeDtypeStruct((16, 128), F32)] + [shape(BLOCK, 512)] * 4,
        scratch_shapes=[
            pltpu.VMEM((BLOCK, 2048), BF16),
            pltpu.VMEM((BLOCK, 512), BF16),
            pltpu.SemaphoreType.DMA((6,)),
        ],
        cost_estimate=cost(2**20, 2**20),
        compiler_params=pltpu.CompilerParams(vmem_limit_bytes=54500 * 1024),
        name="rotate",
    )(small, q, k, v, cosine, sine)


def attend_kernel(rows, const, *refs):
    z = lax.axis_index("z")
    y = lax.axis_index("y")
    q_refs, refs = refs[:4], refs[4:]
    q_ref, sbuf, ebuf, bias = refs[-4:]
    if len(refs) == 11:
        kv_refs, (out_ref, kbuf, vbuf) = refs[:4], refs[4:7]
        for r, ref in enumerate(kv_refs):
            src = lax.rem(y + ORDER[r], 4)
            for j in range(4):
                at = pl.multiple_of(j * 512 + src * 128, 128)
                kbuf[:, pl.ds(at, 128)] = ref[j, :, :128].T
                vbuf[pl.ds(at, 128), :] = ref[j, :, 128:]
    else:
        kbuf, vbuf, out_ref = refs[:3]
    for r, ref in enumerate(q_refs):
        q_ref[lax.rem(z + 4 - r, 4)] = ref[rows, :]

    count = rows.stop - rows.start
    heads = BLOCK // count
    first = lax.broadcasted_iota(jnp.int32, (count, 128), 1) < HEAD_DIM
    zero = jnp.zeros((count, 128), BF16)
    key_at = lax.broadcasted_iota(jnp.int32, (2 * BLOCK, 512), 1)
    query_at = lax.broadcasted_iota(jnp.int32, (2 * BLOCK, 512), 0) % count + rows.start
    bias[...] = jnp.where(key_at <= query_at + y * BLOCK, 0.0, -jnp.inf)
    row_head = lax.broadcasted_iota(jnp.int32, (BLOCK, 1), 0) // count
    steps = [(i, g) for i in range(4) for g in range(4 // heads)]

    def query(n):
        i, g = steps[n]
        qs = [q_ref[i, :, h * 128 : (h + 1) * 128] for h in range(g * heads, (g + 1) * heads)]
        return jnp.concatenate([jnp.where(first, q, zero) for q in qs] + [jnp.where(first, zero, q) for q in qs], 0)

    def score(n, q, t):
        i = steps[n][0]
        s = jnp.dot(q, kbuf[:, t * TILE : (t + 1) * TILE], preferred_element_type=F32)
        edge = t * TILE - i * 512
        if edge >= 0:
            s = s + bias[:, edge : edge + TILE]
        sbuf[n % 3, :, t * TILE : (t + 1) * TILE] = s

    def tops(n):
        reach = (steps[n][0] + 1) * 512
        return jnp.max(sbuf[n % 3, :, :reach], 1, keepdims=True)

    def totals(n):
        reach = (steps[n][0] + 1) * 512
        return 1.0 / jnp.sum(sbuf[n % 3, :, :reach], 1, keepdims=True)

    def blend(n, scale, t):
        at = slice(t * TILE, (t + 1) * TILE)
        w = sbuf[n % 3, :BLOCK, at] * scale[0] - sbuf[n % 3, BLOCK:, at] * scale[1]
        ebuf[n % 2, :, at] = w.astype(BF16)

    def factor(n):
        g = steps[n][1]
        factor = const[g * heads : g * heads + 1, :1]
        if heads == 2:
            factor = jnp.where(row_head == 0, factor, const[g * heads + 1 : g * heads + 2, :1])
        return factor

    def finish(n):
        i, g = steps[n]
        reach = (i + 1) * 512
        acc = jnp.dot(ebuf[n % 2, :, :reach], vbuf[:reach], preferred_element_type=F32)
        square = jnp.mean(acc * acc, 1, keepdims=True)
        acc = acc * (lax.rsqrt(square + NORM_EPS) * OUTPUT_SCALE) * const[8:9]
        acc = acc.astype(BF16)
        for k in range(heads):
            h = g * heads + k
            out_ref[i * count : (i + 1) * count, h * 128 : (h + 1) * 128] = acc[k * count : (k + 1) * count]

    last = len(steps) - 1
    tiles = [(i + 1) * 512 // TILE for i, _ in steps]
    top, scale = {}, {}
    for n in range(-1, last + 2):
        if n < last:
            q = query(n + 1)
        span = max(tiles[k] for k in (n - 1, n, n + 1) if 0 <= k <= last)
        for t in range(span):
            if n < last and t < tiles[n + 1]:
                score(n + 1, q, t)
            if 0 <= n <= last and t < tiles[n]:
                at = slice(t * TILE, (t + 1) * TILE)
                sbuf[n % 3, :, at] = jnp.exp(sbuf[n % 3, :, at] - top[n])
            if n >= 1 and t < tiles[n - 1]:
                blend(n - 1, scale[n - 1], t)
        if n < last:
            top[n + 1] = tops(n + 1)
        if 0 <= n <= last:
            total = totals(n)
            scale[n] = total[:BLOCK], total[BLOCK:] * factor(n)
        if n >= 1:
            finish(n - 1)


def attend(rows, const, q, keys):
    count = rows.stop - rows.start
    outs = [shape(4 * count, 512)]
    if len(keys) == 4:
        outs += [shape(128, SEQ), shape(SEQ, 128)]
    return pl.pallas_call(
        functools.partial(attend_kernel, rows),
        in_specs=[VM] * (5 + len(keys)),
        out_specs=[VM] * len(outs),
        out_shape=outs,
        scratch_shapes=[
            pltpu.VMEM((4, count, 512), BF16),
            pltpu.VMEM((3, 2 * BLOCK, SEQ), F32),
            pltpu.VMEM((2, BLOCK, SEQ), BF16),
            pltpu.VMEM((2 * BLOCK, 512), F32),
        ],
        compiler_params=room(20),
        cost_estimate=cost(2**31, 2**22),
        name="attend",
    )(const, *q, *keys)


ANY = pl.BlockSpec(memory_space=pl.ANY)


def stack_kernel(_, *refs):
    out = refs[-1]
    at = 0
    for ref in refs[:-1]:
        out[at : at + ref.shape[0]] = ref[...]
        at += ref.shape[0]


def stack(after, parts):
    rows = sum(p.shape[0] for p in parts)
    return pl.pallas_call(
        stack_kernel,
        in_specs=[ANY] + [VM] * len(parts),
        out_specs=VM,
        out_shape=shape(rows, parts[0].shape[1]),
        cost_estimate=cost(2**20, 2**20),
        compiler_params=room(4),
        name="stack",
    )(after, *parts)


def columns_kernel(*refs):
    y, x, c = (lax.axis_index(a) for a in "yxc")
    wbuf = refs[-1]
    for k in range(2):
        side = c if k == 0 else 1 - c
        for a in range(4):
            ax = lax.rem(x + ORDER[a], 4)
            for b in range(4):
                by = lax.rem(y + ORDER[b], 4)
                at = pl.multiple_of(by * 256 + ax * 64 + side * 32, 32)
                wbuf[pl.ds(at, 32), :] = refs[4 * k + a][b * 32 : (b + 1) * 32, :]


def columns(parts):
    return pl.pallas_call(
        columns_kernel,
        in_specs=[VM] * 8,
        out_specs=VM,
        out_shape=shape(1024, 2048),
        compiler_params=room(12),
        cost_estimate=cost(2**29, 2**23),
        name="columns",
    )(*parts)


def project_kernel(_, x0, x1, x2, x3, wbuf, *refs):
    outs, xbuf = refs[:4], refs[4]
    z = lax.axis_index("z")
    count = x0.shape[0] // 4
    for r, ref in enumerate((x0, x1, x2, x3)):
        at = pl.multiple_of(lax.rem(z + ORDER[r], 4) * 512, 512)
        for d in range(4):
            row = pl.multiple_of(lax.rem(z + d, 4) * count, count)
            xbuf[d * count : (d + 1) * count, pl.ds(at, 512)] = ref[pl.ds(row, count), :]
    for n in range(4):
        cols = slice(n * 256, (n + 1) * 256)
        part = lax.dot_general(
            xbuf[...], wbuf[cols, :], (((1,), (1,)), ((), ())), preferred_element_type=F32
        ).astype(BF16)
        for d in range(4):
            outs[d][:, cols] = part[d * count : (d + 1) * count]


def project(after, xs, weights):
    rows = xs[0].shape[0]
    return pl.pallas_call(
        project_kernel,
        in_specs=[ANY] + [VM] * 5,
        out_specs=[VM] * 4,
        out_shape=[shape(rows // 4, 1024)] * 4,
        scratch_shapes=[pltpu.VMEM((rows, 2048), BF16)],
        compiler_params=room(16),
        cost_estimate=cost(2**30, 2**22),
        name="project",
    )(after, *xs, weights)


def join_kernel(*refs):
    z = lax.axis_index("z")
    for r in range(4):
        at = pl.multiple_of(lax.rem(z + 4 - r, 4) * 1024, 1024)
        refs[-1][0, :, pl.ds(at, 1024)] = refs[r][...]


def join(p, pieces, whole):
    count = pieces[0].shape[0]
    return pl.pallas_call(
        join_kernel,
        grid=(1,),
        in_specs=[pl.BlockSpec((count, 1024), lambda i: (0, 0))] * 4 + ([] if whole is None else [ANY]),
        out_specs=pl.BlockSpec((1, count, 4096), lambda i: (0, p, 0)),
        out_shape=shape(1, BLOCK, 4096),
        input_output_aliases={} if whole is None else {4: 0},
        cost_estimate=cost(2**18, 2**21),
        compiler_params=room(6),
        name="join",
    )(*pieces, *(() if whole is None else (whole,)))


def shards(queries, keys, values, lambdas, value_gain, out_weight):
    first = ((lax.axis_index("z") * 4 + lax.axis_index("y")) * BLOCK).astype(jnp.int32)
    positions = (first + jnp.arange(BLOCK)).astype(F32)
    freqs = ROPE_BASE ** (-jnp.arange(0, HEAD_DIM, 2, dtype=F32) / HEAD_DIM)
    angles = positions[:, None] * jnp.tile(freqs, 4)[None, :]
    cosine = jnp.cos(angles)
    sign = jnp.where(jnp.arange(128) % HEAD_DIM < HEAD_DIM // 2, -1.0, 1.0).astype(F32)
    sine = jnp.sin(angles) * sign[None, :]
    small = jnp.stack([jnp.pad(lambdas, (0, 128 - lambdas.shape[0])), value_gain])
    wy = line("y", out_weight.T)
    kv_split, const, *q_split = rotate(small, queries, keys, values, cosine, sine)

    kv_line = lax.all_to_all(kv_split, "z", 0, 0)
    kv_all = line("y", kv_line)
    q = [q_split[0]] + [hop("z", r, q_split[r]) for r in (1, 2, 3)]

    wy = stack(kv_line, wy)
    wx = line("x", wy)
    wc = tuple(lax.ppermute(p, "c", [(0, 1), (1, 0)]) for p in wx)
    weights = columns(wx + wc)

    count = BLOCK // PARTS
    keys_all = kv_all
    heads = []
    for p in range(PARTS):
        got, *whole = attend(slice(p * count, (p + 1) * count), const, q, keys_all)
        keys_all = whole or keys_all
        heads.append(got)
    out = None
    for p in range(PARTS):
        got = line("z", heads[p])
        sent = project(heads[-1], got, weights)
        got = [sent[0]] + [hop("z", r, sent[r]) for r in (1, 2, 3)]
        out = join(p, got, out)
    return out


def solution(mesh):
    fine = Mesh(mesh.devices.reshape(4, 4, 4, 2), ("z", "y", "x", "c"))
    tokens = P(("x", "c"), ("z", "y"), None)
    return jax.shard_map(
        shards,
        mesh=fine,
        in_specs=(tokens, tokens, tokens, P(), P(), P(None, ("z", "y", "x", "c"))),
        out_specs=tokens,
        check_vma=False,
    )
```

```python
import functools

import jax
import jax.numpy as jnp
from jax import lax
from jax.experimental import pallas as pl
from jax.experimental.pallas import tpu as pltpu
from jax.sharding import Mesh
from jax.sharding import PartitionSpec as P


F32 = jnp.float32
BF16 = jnp.bfloat16
HEAD_DIM = 64
ROPE_BASE = 500000.0
OUTPUT_SCALE = 0.8
NORM_EPS = 1e-05
BLOCK = 128
SEQ = 2048
TILE = 256
PARTS = (slice(0, 64), slice(64, 128))

VM = pl.BlockSpec(memory_space=pltpu.VMEM)
SM = pl.BlockSpec(memory_space=pltpu.SMEM)


def cost(flops, size):
    return pl.CostEstimate(flops=flops, bytes_accessed=size, transcendentals=0)


def room(mib):
    return pltpu.CompilerParams(vmem_limit_bytes=mib * 1024 * 1024)


def shape(*dims):
    return jax.ShapeDtypeStruct(dims, BF16)


def hop(axis, step, x):
    return lax.ppermute(x, axis, [(i, (i + step) % 4) for i in range(4)])


def line(axis, x):
    return x, hop(axis, 1, x), hop(axis, 3, x), hop(axis, 2, x)


ORDER = (0, 3, 1, 2)


HBM = pl.BlockSpec(memory_space=pltpu.HBM)


def rotate_kernel(
    small_ref, q_hbm, k_hbm, v_hbm, w_hbm, cos_ref, sin_ref, const_out, w_out, q0, q1, q2, q3, kv0, kv1, kv2, kv3, q_ref, k_ref, v_ref, sems
):
    z = lax.axis_index("z")
    copies = [pltpu.make_async_copy(k_hbm.at[0], k_ref, sems.at[0])]
    copies.append(pltpu.make_async_copy(v_hbm.at[0], v_ref, sems.at[1]))
    copies.append(pltpu.make_async_copy(q_hbm.at[0], q_ref, sems.at[2]))
    copies.append(pltpu.make_async_copy(w_hbm, w_out, sems.at[3]))
    for copy in copies:
        copy.start()
    cosine = cos_ref[...]
    sine = sin_ref[...]
    lane = lax.broadcasted_iota(jnp.int32, (BLOCK, 128), 1)
    low = (lane % HEAD_DIM) < HEAD_DIM // 2

    def turn(x):
        x = x.astype(F32)
        other = jnp.where(low, pltpu.roll(x, 96, 1), pltpu.roll(x, 32, 1))
        return (x * cosine + other * sine).astype(BF16)

    copies[0].wait()
    copies[1].wait()
    for r, kv_out in enumerate((kv0, kv1, kv2, kv3)):
        at = pl.multiple_of(lax.rem(z + r, 4) * 128, 128)
        kv_out[:, :128] = turn(k_ref[:, pl.ds(at, 128)])
        kv_out[:, 128:] = v_ref[:, pl.ds(at, 128)]
    copies[2].wait()
    for r, q_out in enumerate((q0, q1, q2, q3)):
        group = lax.rem(z + r, 4) * 512
        for h in range(4):
            at = pl.multiple_of(group + h * 128, 128)
            q_out[:, h * 128 : (h + 1) * 128] = turn(q_ref[:, pl.ds(at, 128)]) * BF16(0.125)
    at = lax.broadcasted_iota(jnp.int32, (8, 128), 1) - lax.broadcasted_iota(jnp.int32, (8, 128), 0)
    own = jnp.where(at == z * 4, jnp.broadcast_to(small_ref[1:], (8, 128)), 0.0)
    const_out[:8] = jnp.broadcast_to(jnp.sum(own, 1, keepdims=True), (8, 128))
    const_out[8:] = jnp.broadcast_to(small_ref[:1], (8, 128))
    copies[3].wait()


def rotate(small, q, k, v, w, cosine, sine):
    return pl.pallas_call(
        rotate_kernel,
        in_specs=[VM] + [HBM] * 4 + [VM] * 2,
        out_specs=[VM] * 10,
        out_shape=[jax.ShapeDtypeStruct((16, 128), F32), shape(*w.shape)]
        + [shape(BLOCK, 512)] * 4
        + [shape(BLOCK, 256)] * 4,
        scratch_shapes=[
            pltpu.VMEM((BLOCK, 2048), BF16),
            pltpu.VMEM((BLOCK, 512), BF16),
            pltpu.VMEM((BLOCK, 512), BF16),
            pltpu.SemaphoreType.DMA((4,)),
        ],
        cost_estimate=cost(2**20, 2**20),
        compiler_params=pltpu.CompilerParams(vmem_limit_bytes=54200 * 1024),
        name="rotate",
    )(small, q, k, v, w, cosine, sine)


def attend_kernel(rows, const, *refs):
    z = lax.axis_index("z")
    y = lax.axis_index("y")
    q_refs, refs = refs[:4], refs[4:]
    q_ref, sbuf, ebuf, bias = refs[-4:]
    if len(refs) == 11:
        kv_refs, (out_ref, kbuf, vbuf) = refs[:4], refs[4:7]
        for r, ref in enumerate(kv_refs):
            src = lax.rem(y + ORDER[r], 4)
            for j in range(4):
                at = pl.multiple_of(lax.rem(z + 4 - j, 4) * 512 + src * 128, 128)
                kbuf[:, pl.ds(at, 128)] = ref[j, :, :128].T
                vbuf[pl.ds(at, 128), :] = ref[j, :, 128:]
    else:
        kbuf, vbuf, out_ref = refs[:3]
    for r, ref in enumerate(q_refs):
        q_ref[lax.rem(z + 4 - r, 4)] = ref[rows, :]

    count = rows.stop - rows.start
    heads = BLOCK // count
    span = heads * count
    first = lax.broadcasted_iota(jnp.int32, (count, 128), 1) < HEAD_DIM
    zero = jnp.zeros((count, 128), BF16)
    key_at = lax.broadcasted_iota(jnp.int32, (2 * span, 512), 1)
    query_at = lax.broadcasted_iota(jnp.int32, (2 * span, 512), 0) % count + rows.start
    bias[...] = jnp.where(key_at <= query_at + y * BLOCK, 0.0, -jnp.inf)
    row_head = lax.broadcasted_iota(jnp.int32, (span, 1), 0) // count
    steps = [(i, g) for i in range(4) for g in range(4 // heads)]

    def query(n):
        i, g = steps[n]
        qs = [q_ref[i, :, h * 128 : (h + 1) * 128] for h in range(g * heads, (g + 1) * heads)]
        return jnp.concatenate([jnp.where(first, q, zero) for q in qs] + [jnp.where(first, zero, q) for q in qs], 0)

    def score(n, q, t):
        i = steps[n][0]
        s = jnp.dot(q, kbuf[:, t * TILE : (t + 1) * TILE], preferred_element_type=F32)
        edge = t * TILE - i * 512
        if edge >= 0:
            s = s + bias[:, edge : edge + TILE]
        sbuf[n % 3, :, t * TILE : (t + 1) * TILE] = s

    def tops(n):
        reach = (steps[n][0] + 1) * 512
        return jnp.max(sbuf[n % 3, :, :reach], 1, keepdims=True)

    def totals(n):
        reach = (steps[n][0] + 1) * 512
        return 1.0 / jnp.sum(sbuf[n % 3, :, :reach], 1, keepdims=True)

    def blend(n, scale, t):
        at = slice(t * TILE, (t + 1) * TILE)
        w = sbuf[n % 3, :span, at] * scale[0] - sbuf[n % 3, span:, at] * scale[1]
        ebuf[n % 2, :, at] = w.astype(BF16)

    def factor(n):
        g = steps[n][1]
        value = const[g * heads : g * heads + 1, :1]
        for k in range(1, heads):
            value = jnp.where(row_head < k, value, const[g * heads + k : g * heads + k + 1, :1])
        return value

    def finish(n):
        i, g = steps[n]
        reach = (i + 1) * 512
        acc = jnp.dot(ebuf[n % 2, :, :reach], vbuf[:reach], preferred_element_type=F32)
        square = jnp.mean(acc * acc, 1, keepdims=True)
        acc = acc * (lax.rsqrt(square + NORM_EPS) * OUTPUT_SCALE) * const[8:9]
        acc = acc.astype(BF16)
        for k in range(heads):
            h = g * heads + k
            out_ref[i * count : (i + 1) * count, h * 128 : (h + 1) * 128] = acc[k * count : (k + 1) * count]

    last = len(steps) - 1
    tiles = [(i + 1) * 512 // TILE for i, _ in steps]
    top, scale = {}, {}
    for n in range(-1, last + 2):
        if n < last:
            q = query(n + 1)
        longest = max(tiles[k] for k in (n - 1, n, n + 1) if 0 <= k <= last)
        for t in range(longest):
            if n < last and t < tiles[n + 1]:
                score(n + 1, q, t)
            if 0 <= n <= last and t < tiles[n]:
                at = slice(t * TILE, (t + 1) * TILE)
                sbuf[n % 3, :, at] = jnp.exp(sbuf[n % 3, :, at] - top[n])
            if n >= 1 and t < tiles[n - 1]:
                blend(n - 1, scale[n - 1], t)
        if n < last:
            top[n + 1] = tops(n + 1)
        if 0 <= n <= last:
            total = totals(n)
            scale[n] = total[:span], total[span:] * factor(n)
        if n >= 1:
            finish(n - 1)


def attend(rows, const, q, keys):
    count = rows.stop - rows.start
    span = BLOCK // count * count
    outs = [shape(4 * count, 512)]
    if len(keys) == 4:
        outs += [shape(128, SEQ), shape(SEQ, 128)]
    return pl.pallas_call(
        functools.partial(attend_kernel, rows),
        in_specs=[VM] * (5 + len(keys)),
        out_specs=[VM] * len(outs),
        out_shape=outs,
        scratch_shapes=[
            pltpu.VMEM((4, count, 512), BF16),
            pltpu.VMEM((3, 2 * span, SEQ), F32),
            pltpu.VMEM((2, span, SEQ), BF16),
            pltpu.VMEM((2 * span, 512), F32),
        ],
        compiler_params=room(20),
        cost_estimate=cost(2**31, 2**22),
        name="attend",
    )(const, *q, *keys)


ANY = pl.BlockSpec(memory_space=pl.ANY)


def stack_kernel(*refs):
    out = refs[-1]
    at = 0
    for ref in refs[:-1]:
        out[at : at + ref.shape[0]] = ref[...]
        at += ref.shape[0]


def stack(parts):
    rows = sum(p.shape[0] for p in parts)
    return pl.pallas_call(
        stack_kernel,
        in_specs=[VM] * len(parts),
        out_specs=VM,
        out_shape=shape(rows, *parts[0].shape[1:]),
        cost_estimate=cost(2**20, 2**20),
        compiler_params=room(4),
    )(*parts)


def columns_kernel(*refs):
    y, x, c = (lax.axis_index(a) for a in "yxc")
    wbuf = refs[-1]
    for k in range(2):
        side = c if k == 0 else 1 - c
        for a in range(4):
            ax = lax.rem(x + ORDER[a], 4)
            for b in range(4):
                by = lax.rem(y + ORDER[b], 4)
                at = pl.multiple_of(by * 256 + ax * 64 + side * 32, 32)
                wbuf[pl.ds(at, 32), :] = refs[4 * k + a][b * 32 : (b + 1) * 32, :]


def columns(parts):
    return pl.pallas_call(
        columns_kernel,
        in_specs=[VM] * 8,
        out_specs=VM,
        out_shape=shape(1024, 2048),
        compiler_params=room(12),
        cost_estimate=cost(2**29, 2**23),
        name="columns",
    )(*parts)


def project_kernel(_, x0, x1, x2, x3, wbuf, *refs):
    outs, xbuf = refs[:4], refs[4]
    z = lax.axis_index("z")
    count = x0.shape[0] // 4
    for r, ref in enumerate((x0, x1, x2, x3)):
        at = pl.multiple_of(lax.rem(z + ORDER[r], 4) * 512, 512)
        for d in range(4):
            row = pl.multiple_of(lax.rem(z + d, 4) * count, count)
            xbuf[d * count : (d + 1) * count, pl.ds(at, 512)] = ref[pl.ds(row, count), :]
    for n in range(4):
        cols = slice(n * 256, (n + 1) * 256)
        part = lax.dot_general(
            xbuf[...], wbuf[cols, :], (((1,), (1,)), ((), ())), preferred_element_type=F32
        ).astype(BF16)
        for d in range(4):
            outs[d][:, cols] = part[d * count : (d + 1) * count]


def project(after, xs, weights):
    rows = xs[0].shape[0]
    return pl.pallas_call(
        project_kernel,
        in_specs=[ANY] + [VM] * 5,
        out_specs=[VM] * 4,
        out_shape=[shape(rows // 4, 1024)] * 4,
        scratch_shapes=[pltpu.VMEM((rows, 2048), BF16)],
        compiler_params=room(16),
        cost_estimate=cost(2**30, 2**22),
        name="project",
    )(after, *xs, weights)


def join_kernel(rows, *refs):
    z = lax.axis_index("z")
    out, sems = refs[-2:]
    copies = []
    for r in range(4):
        at = pl.multiple_of(lax.rem(z + 4 - r, 4) * 1024, 1024)
        to = out.at[0, pl.ds(rows.start, rows.stop - rows.start), pl.ds(at, 1024)]
        copies.append(pltpu.make_async_copy(refs[r], to, sems.at[r]))
        copies[-1].start()
    for copy in copies:
        copy.wait()


def join(rows, pieces, whole):
    return pl.pallas_call(
        functools.partial(join_kernel, rows),
        in_specs=[VM] * 4 + ([] if whole is None else [ANY]),
        out_specs=ANY,
        out_shape=shape(1, BLOCK, 4096),
        scratch_shapes=[pltpu.SemaphoreType.DMA((4,))],
        input_output_aliases={} if whole is None else {4: 0},
        cost_estimate=cost(2**18, 2**21),
        compiler_params=room(6),
        name="join",
    )(*pieces, *(() if whole is None else (whole,)))


def shards(queries, keys, values, lambdas, value_gain, out_weight):
    first = ((lax.axis_index("z") * 4 + lax.axis_index("y")) * BLOCK).astype(jnp.int32)
    positions = (first + jnp.arange(BLOCK)).astype(F32)
    freqs = ROPE_BASE ** (-jnp.arange(0, HEAD_DIM, 2, dtype=F32) / HEAD_DIM)
    angles = positions[:, None] * jnp.tile(freqs, 4)[None, :]
    cosine = jnp.cos(angles)
    sign = jnp.where(jnp.arange(128) % HEAD_DIM < HEAD_DIM // 2, -1.0, 1.0).astype(F32)
    sine = jnp.sin(angles) * sign[None, :]
    small = jnp.concatenate([value_gain, lambdas, jnp.zeros(128 - lambdas.shape[0], F32)]).reshape(2, 128)
    got = rotate(small, queries, keys, values, out_weight.T, cosine, sine)
    const, wt, q_split, kv_split = got[0], got[1], got[2:6], got[6:]

    kv_line = [kv_split[0][None]] + [hop("z", r, kv_split[r])[None] for r in (1, 2, 3)]
    wy = line("y", wt)
    kv_line = stack(kv_line)
    kv_all = line("y", kv_line)
    q = [q_split[0]] + [hop("z", r, q_split[r]) for r in (1, 2, 3)]
    wy = stack(wy)
    wx = line("x", wy)
    wc = tuple(lax.ppermute(p, "c", [(0, 1), (1, 0)]) for p in wx[1:])
    wc = (lax.ppermute(wy, "c", [(0, 1), (1, 0)]),) + wc
    weights = columns(wx + wc)

    keys_all = kv_all
    heads = []
    for rows in PARTS:
        got, *built = attend(rows, const, q, keys_all)
        keys_all = built or keys_all
        heads.append(got)
    out = None
    for p, rows in enumerate(PARTS):
        got = line("z", heads[p])
        sent = project(heads[-1], got, weights)
        got = [sent[0]] + [hop("z", r, sent[r]) for r in (1, 2, 3)]
        out = join(rows, got, out)
    return out


def solution(mesh):
    fine = Mesh(mesh.devices.reshape(4, 4, 4, 2), ("z", "y", "x", "c"))
    tokens = P(("x", "c"), ("z", "y"), None)
    return jax.shard_map(
        shards,
        mesh=fine,
        in_specs=(tokens, tokens, tokens, P(), P(), P(None, ("z", "y", "x", "c"))),
        out_specs=tokens,
        check_vma=False,
    )
```
